32 devices in a mesh: ra: 16 (over z, y, x), cb: 2 (over core).
Axes of the slice: x: 2, y: 2, z: 4, core: 2. Of those that a mesh axis runs over, the one named last changes fastest.
Arguments:
- activations: bfloat16 [768, 4096], P('ra', 'cb'), may hold values from -230 to 230
- gain_first: float32 [4096], P('cb'), may hold values from 0.1 to 1.9
- gate_weight: float32 [11264, 4096], P('ra', 'cb'), may hold values from -0.125 to 0.125
- gate_scale: float32 [11264], P('ra'), may hold values from 0.5 to 2
- up_weight: float32 [11264, 4096], P('ra', 'cb'), may hold values from -0.125 to 0.125
- up_scale: float32 [11264], P('ra'), may hold values from 0.5 to 2
- down_weight: float32 [11264, 4096], P('ra', 'cb'), may hold values from -0.0546875 to 0.0546875
- down_scale: float32 [4096], P('cb'), may hold values from 0.35 to 2.8
- gain_second: float32 [4096], P('cb'), may hold values from 0.1 to 1.9
Outputs:
- normed: bfloat16 [768, 4096], P('ra', 'cb')
The draws below stay inside these ranges and needn't reach their ends.
All inputs are finite; a program needn't handle non-finite values.
Results may differ from the reference program's by a relative error of at most 0.011.
Values may be sent and summed in bfloat16 or wider, within the bound.
A program may use at most 64 MiB of HBM per device.

```python
import math
import jax
import jax.numpy as jnp
from jax import lax

D = 4096
FF = 11264
TOKENS = 768


def draw_activations(key, part):
    first, second, third = jax.random.split(jax.random.fold_in(key, 17), 3)
    columns = jnp.arange(D, dtype=jnp.float32) / D
    column_factor = jnp.exp(jnp.log(4.0) * (columns - 0.5)) * jax.random.uniform(second, (D,), jnp.float32, 0.6, 1.4)
    base = jnp.clip(jax.random.normal(first, (TOKENS, D), jnp.float32), -5.0, 5.0)
    rows = jnp.exp(jax.random.uniform(third, (TOKENS, 1), jnp.float32, 0.0, jnp.log(10.0)))
    return (base * rows * column_factor).astype(jnp.bfloat16)


def draw_down_scale(key, part):
    columns = jnp.arange(D, dtype=jnp.float32) / D
    rising = jnp.exp(jnp.log(4.0) * (columns - 0.5))
    noise = jax.random.uniform(jax.random.fold_in(key, 29), (D,), jnp.float32, 0.7, 1.4)
    return rising * noise


def raised(drawn, stream_key, source, target, blocks, factor):
    owner, partner = [(jnp.arange(drawn.shape[position]) // (drawn.shape[position] // blocks)).reshape([-1 if axis == position else 1 for axis in range(drawn.ndim)]) for position in (source, target)]
    chosen = jax.random.permutation(stream_key, blocks)[partner]
    strong = (owner == chosen) | (owner == (partner + blocks // 2) % blocks)
    return jnp.where(strong, factor * drawn, drawn)


def block_levels(own_key, extent, pieces, low, largest):
    factor_of, own = 1.0, jax.random.fold_in(own_key, 6)
    for position, shards_of in pieces:
        draws = jnp.exp(jax.random.uniform(jax.random.fold_in(own, position), (shards_of,), jnp.float32, low / len(pieces), largest / len(pieces)))
        factor_of = factor_of * jnp.repeat(draws, extent[position] // shards_of).reshape([-1 if axis == position else 1 for axis in range(len(extent))])
    return factor_of


def centred(rng, extent, spread, reach, shards=(), held_as=jnp.bfloat16):
    entries = jax.random.normal(rng, extent, jnp.float32) * spread
    if len(shards) > 0:
        entries = block_levels(rng, extent, shards, -0.22, 0.18) * entries
    return jnp.clip(entries, min=-reach, max=reach).astype(held_as)


def bell_draw_with(rng, dims, width, most, cuts, heavy, kind=jnp.bfloat16):
    drawn = width * jax.random.normal(rng, dims, jnp.float32)
    if cuts:
        drawn = drawn * block_levels(rng, dims, cuts, -0.22, 0.18)
    return jnp.clip(raised(drawn, jax.random.fold_in(rng, 3), *heavy), -most, most).astype(kind)


def setup_inputs(seed: int = 0) -> dict:
    seeds = jax.random.split(jax.random.key(seed), 10)
    activations = draw_activations(jax.random.fold_in(seeds[9], 71), 0)
    gain_first = jnp.clip(1.0 + 0.18 * jax.random.normal(seeds[1], (D,), jnp.float32), 0.1, 1.9)
    gate_weight = bell_draw_with(seeds[2], (FF, D), D ** -0.5, 0.125, ((0, 16), (1, 2)), (1, 0, 16, 2.0), jnp.float32)
    gate_scale = jnp.clip(jnp.exp(math.log(2.0) - 1.3862944 * jax.random.uniform(seeds[3], (FF,), jnp.float32) ** block_levels(seeds[3], (FF,), ((0, 16),), -0.2, 0.2)), 0.5, 2.0)
    up_weight = bell_draw_with(seeds[4], (FF, D), D ** -0.5, 0.125, ((0, 16), (1, 2)), (1, 0, 16, 2.0), jnp.float32)
    up_scale = jnp.clip(jnp.exp(math.log(2.0) - 1.3862944 * jax.random.uniform(seeds[5], (FF,), jnp.float32) ** block_levels(seeds[5], (FF,), ((0, 16),), -0.2, 0.2)), 0.5, 2.0)
    down_weight = centred(seeds[6], (FF, D), FF ** -0.5, 0.0546875, ((0, 16), (1, 2)), jnp.float32)
    down_scale = draw_down_scale(jax.random.fold_in(seeds[9], 71), 0)
    gain_second = jnp.clip(1.0 + 0.18 * jax.random.normal(seeds[8], (D,), jnp.float32), 0.1, 1.9)
    return {"activations": activations, "gain_first": gain_first, "gate_weight": gate_weight, "gate_scale": gate_scale, "up_weight": up_weight, "up_scale": up_scale, "down_weight": down_weight, "down_scale": down_scale, "gain_second": gain_second}


EPS = 1e-06

def reference(activations, gain_first, gate_weight, gate_scale, up_weight, up_scale, down_weight, down_scale, gain_second):
    inputs = activations.astype(jnp.float32)
    rscale_first = lax.rsqrt(lax.optimization_barrier(jnp.mean(inputs * inputs, axis=1)) + EPS)[:, None]
    scaled = (inputs * gain_first).astype(jnp.bfloat16)
    gate_raw = jnp.dot(scaled, gate_weight.astype(jnp.bfloat16).T, preferred_element_type=jnp.float32)
    up_raw = jnp.dot(scaled, up_weight.astype(jnp.bfloat16).T, preferred_element_type=jnp.float32)
    gate = gate_raw * rscale_first * gate_scale
    up = up_raw * rscale_first * up_scale
    hidden = (jax.nn.silu(gate) * up).astype(jnp.bfloat16)
    mixed = jnp.dot(hidden, down_weight.astype(jnp.bfloat16), preferred_element_type=jnp.float32) * down_scale
    stream = 0.1 * inputs + mixed
    rscale_second = lax.rsqrt(lax.optimization_barrier(jnp.mean(stream * stream, axis=1)) + EPS)[:, None]
    return (stream * rscale_second * gain_second).astype(jnp.bfloat16)
```

```python
import functools

import jax
import jax.numpy as jnp
from jax import lax
from jax.experimental import pallas as pl
from jax.experimental.pallas import tpu as pltpu
from jax.sharding import PartitionSpec as P

EPS = 1e-06
MESH = pl.DeviceIdType.MESH
F32 = jnp.float32
BF16 = jnp.bfloat16


def flip(index, mask):
    bit = 1
    while bit <= mask:
        if mask & bit:
            index = index + (1 - 2 * ((index // bit) % 2)) * bit
        bit *= 2
    return index


def kernel(
    planes,
    features,
    x_ref,
    gain_ref,
    gate_hbm,
    gate_scale_ref,
    up_hbm,
    up_scale_ref,
    down_hbm,
    down_scale_ref,
    gain2_ref,
    out_ref,
    wide,
    gate_w,
    up_w,
    down_w,
    xg,
    scaled,
    hidden,
    part,
    ex_send,
    ex_recv,
    sq_send,
    sq_recv,
    keep_a,
    keep_b,
    send_a,
    send_b,
    recv_a,
    recv_b,
    send2_a,
    send2_b,
    recv2_a,
    recv2_b,
    own_sum,
    z_send,
    z_recv,
    last_send,
    last_recv,
    w_sem,
    ssem,
    rsem,
):
    ra = lax.axis_index("ra")
    cb = lax.axis_index("cb")
    rows, width = x_ref.shape
    half = width // 2
    x_peer = (flip(ra, 1), cb)
    y_peer = (flip(ra, 2), cb)
    z_peers = [None] + [(flip(ra, 4 * k), cb) for k in range(1, planes)]
    core_peer = (ra, flip(cb, 1))
    first, second = pl.ds(0, half), pl.ds(half, half)

    loads = []
    for i, src in enumerate((gate_hbm, up_hbm, down_hbm)):
        load = pltpu.make_async_copy(src, wide.at[i], w_sem.at[i])
        load.start()
        loads.append(load)

    barrier = pltpu.get_barrier_semaphore()
    peers = [x_peer, y_peer, core_peer] + z_peers[1:]
    for peer in peers:
        pl.semaphore_signal(barrier, inc=1, device_id=peer, device_id_type=MESH)
    pl.semaphore_wait(barrier, len(peers))

    copies = {}

    def send(name, k, src, dst, peer):
        slot = len(copies)
        copy = pltpu.make_async_remote_copy(
            src_ref=src,
            dst_ref=dst,
            send_sem=ssem.at[slot],
            recv_sem=rsem.at[slot],
            device_id=peer,
            device_id_type=MESH,
        )
        copy.start()
        copies[name, k] = copy

    def arrived(name, k):
        copies[name, k].wait_recv()

    def spread(k):
        src = x_ref if k == 0 else xg.at[k, 0]
        if k:
            arrived("z", k)
        send("gx", k, src, xg.at[k, 1], x_peer)
        send("gy", k, src, xg.at[k, 2], y_peer)

    def forward(k):
        arrived("gx", k)
        send("fy", k, xg.at[k, 1, :, second], xg.at[k, 3, :, second], y_peer)
        arrived("gy", k)
        send("fx", k, xg.at[k, 2, :, first], xg.at[k, 3, :, first], x_peer)

    nt = (((1,), (1,)), ((), ()))

    def gate_up(k):
        arrived("fx", k)
        arrived("fy", k)

        def prepare(s, carry):
            block = xg[k, s].astype(F32)
            squares = jnp.sum(block * block, axis=1, keepdims=True)
            sq_send[k, s] = jnp.broadcast_to(squares, (rows, 128))
            scaled[s] = (block * gain_ref[...]).astype(BF16)
            return carry

        lax.fori_loop(0, 4, prepare, 0)
        send("sq", k, sq_send.at[k], sq_recv.at[k], core_peer)
        tokens = scaled[...].reshape(4 * rows, width)
        for i, w in enumerate((gate_w, up_w)):
            product = lax.dot_general(tokens, w[...], nt, preferred_element_type=F32)
            part[k, i] = product
            ex_send[k, i] = product.astype(BF16)
            send(("ex", i), k, ex_send.at[k, i], ex_recv.at[k, i], core_peer)

    def down(k):
        arrived("sq", k)
        arrived(("ex", 0), k)
        arrived(("ex", 1), k)

        for s in range(4):
            here = slice(s * rows, (s + 1) * rows)
            squares = (sq_send[k, s] + sq_recv[k, s])[:, :1]
            rscale = lax.rsqrt(squares / features + EPS)
            gate = (part[k, 0, here] + ex_recv[k, 0, here].astype(F32)) * rscale * gate_scale_ref[...]
            up = (part[k, 1, here] + ex_recv[k, 1, here].astype(F32)) * rscale * up_scale_ref[...]
            hidden[here] = (gate / (1.0 + jnp.exp(-gate)) * up).astype(BF16)
        units = hidden[...]
        prod = jnp.dot(units, down_w[:, :half], preferred_element_type=F32)
        for dy in range(2):
            low = 2 * dy * rows
            keep_a[k, dy] = prod[low : low + rows]
            send_a[k, dy] = prod[low + rows : low + 2 * rows].astype(BF16)
        send("a1", k, send_a.at[k], recv_a.at[k], x_peer)
        prod = jnp.dot(units, down_w[:, half:], preferred_element_type=F32)
        for dx in range(2):
            low = dx * rows
            keep_b[k, dx] = prod[low : low + rows]
            low += 2 * rows
            send_b[k, dx] = prod[low : low + rows].astype(BF16)
        send("b1", k, send_b.at[k], recv_b.at[k], y_peer)

    def reduce_one(k):
        arrived("a1", k)
        send2_a[k] = (keep_a[k, 1] + recv_a[k, 1].astype(F32)).astype(BF16)
        send("a2", k, send2_a.at[k], recv2_a.at[k], y_peer)
        arrived("b1", k)
        send2_b[k] = (keep_b[k, 1] + recv_b[k, 1].astype(F32)).astype(BF16)
        send("b2", k, send2_b.at[k], recv2_b.at[k], x_peer)

    def reduce_two(k):
        arrived("a2", k)
        sum_a = keep_a[k, 0] + recv_a[k, 0].astype(F32) + recv2_a[k].astype(F32)
        arrived("b2", k)
        sum_b = keep_b[k, 0] + recv_b[k, 0].astype(F32) + recv2_b[k].astype(F32)
        if k == 0:
            own_sum[:, :half] = sum_a
            own_sum[:, half:] = sum_b
        else:
            z_send[k, :, :half] = sum_a.astype(BF16)
            z_send[k, :, half:] = sum_b.astype(BF16)
            send("zs", k, z_send.at[k], z_recv.at[k], z_peers[k])

    def narrow(i, target):
        loads[i].wait()
        step = 64

        def body(j, carry):
            here = pl.ds(pl.multiple_of(j * step, step), step)
            target[here] = wide[i, here].astype(BF16)
            return carry

        lax.fori_loop(0, target.shape[0] // step, body, 0)

    spread(0)
    for k in range(1, planes):
        send("z", k, x_ref, xg.at[k, 0], z_peers[k])
    xg[0, 0] = x_ref[...]
    narrow(0, gate_w)
    forward(0)
    spread(1)
    narrow(1, up_w)
    gate_up(0)
    narrow(2, down_w)
    order = list(range(1, planes))
    for k in order:
        forward(k)
        if k + 1 < planes:
            spread(k + 1)
        if k > 1:
            down(k - 1)
        gate_up(k)
    down(planes - 1)
    late = order + [0]
    reduce_one(1)
    down(0)
    for at in range(1, planes):
        reduce_one(late[at])
        reduce_two(late[at - 1])
    reduce_two(0)

    total = own_sum[...]
    for k in range(1, planes):
        arrived("zs", k)
        total = total + z_recv[k].astype(F32)
    stream = 0.1 * x_ref[...].astype(F32) + total * down_scale_ref[...]
    own_sum[...] = stream
    last_send[...] = jnp.broadcast_to(
        jnp.sum(stream * stream, axis=1, keepdims=True), last_send.shape
    )
    send("last", 0, last_send, last_recv, core_peer)
    arrived("last", 0)
    both = (last_send[...] + last_recv[...])[:, :1]
    rscale = lax.rsqrt(both / features + EPS)
    out_ref[...] = (own_sum[...] * rscale * gain2_ref[...]).astype(BF16)
    for copy in copies.values():
        copy.wait_send()


def fused(
    planes,
    activations,
    gain_first,
    gate_weight,
    gate_scale,
    up_weight,
    up_scale,
    down_weight,
    down_scale,
    gain_second,
):
    rows, width = activations.shape
    units = gate_weight.shape[0]
    half = width // 2
    group = 4 * rows
    n_copies = 16 * planes
    vmem = pl.BlockSpec(memory_space=pltpu.VMEM)
    hbm = pl.BlockSpec(memory_space=pl.ANY)
    scratch = [
        pltpu.VMEM((3, units, width), F32),
        pltpu.VMEM((units, width), BF16),
        pltpu.VMEM((units, width), BF16),
        pltpu.VMEM((units, width), BF16),
        pltpu.VMEM((planes, 4, rows, width), BF16),
        pltpu.VMEM((4, rows, width), BF16),
        pltpu.VMEM((group, units), BF16),
        pltpu.VMEM((planes, 2, group, units), F32),
        pltpu.VMEM((planes, 2, group, units), BF16),
        pltpu.VMEM((planes, 2, group, units), BF16),
        pltpu.VMEM((planes, 4, rows, 128), F32),
        pltpu.VMEM((planes, 4, rows, 128), F32),
        pltpu.VMEM((planes, 2, rows, half), F32),
        pltpu.VMEM((planes, 2, rows, half), F32),
        pltpu.VMEM((planes, 2, rows, half), BF16),
        pltpu.VMEM((planes, 2, rows, half), BF16),
        pltpu.VMEM((planes, 2, rows, half), BF16),
        pltpu.VMEM((planes, 2, rows, half), BF16),
        pltpu.VMEM((planes, rows, half), BF16),
        pltpu.VMEM((planes, rows, half), BF16),
        pltpu.VMEM((planes, rows, half), BF16),
        pltpu.VMEM((planes, rows, half), BF16),
        pltpu.VMEM((rows, width), F32),
        pltpu.VMEM((planes, rows, width), BF16),
        pltpu.VMEM((planes, rows, width), BF16),
        pltpu.VMEM((rows, 128), F32),
        pltpu.VMEM((rows, 128), F32),
        pltpu.SemaphoreType.DMA((3,)),
        pltpu.SemaphoreType.DMA((n_copies,)),
        pltpu.SemaphoreType.DMA((n_copies,)),
    ]
    return pl.pallas_call(
        functools.partial(kernel, planes, width * 2),
        out_shape=jax.ShapeDtypeStruct((rows, width), BF16),
        in_specs=[vmem, vmem, hbm, vmem, hbm, vmem, hbm, vmem, vmem],
        out_specs=vmem,
        scratch_shapes=scratch,
        compiler_params=pltpu.CompilerParams(
            collective_id=0, has_side_effects=True, vmem_limit_bytes=60 * 1024 * 1024
        ),
    )(
        activations,
        gain_first[None, :],
        gate_weight,
        gate_scale[None, :],
        up_weight,
        up_scale[None, :],
        down_weight,
        down_scale[None, :],
        gain_second[None, :],
    )


def plain(
    activations,
    gain_first,
    gate_weight,
    gate_scale,
    up_weight,
    up_scale,
    down_weight,
    down_scale,
    gain_second,
):
    inputs = activations.astype(F32)
    features = activations.shape[1] * lax.axis_size("cb")
    gate_local = gate_weight.astype(BF16)
    up_local = up_weight.astype(BF16)
    down_local = down_weight.astype(BF16)
    gathered = lax.all_gather(activations, "ra", axis=0, tiled=True)
    wide_rows = gathered.astype(F32)
    row_squares = jnp.sum(wide_rows * wide_rows, axis=1)
    scaled = (wide_rows * gain_first).astype(BF16)
    contract = (((1,), (1,)), ((), ()))
    squares = lax.psum(row_squares, "cb")
    gate_part = lax.dot_general(gate_local, scaled, contract, preferred_element_type=F32)
    up_part = lax.dot_general(up_local, scaled, contract, preferred_element_type=F32)
    gate_sum, up_sum = lax.psum((gate_part, up_part), "cb")
    rscale_first = lax.rsqrt(squares / features + EPS)[None, :]
    gate_full = gate_sum * rscale_first * gate_scale[:, None]
    up_full = up_sum * rscale_first * up_scale[:, None]
    hidden = (jax.nn.silu(gate_full) * up_full).astype(BF16)
    mixed = lax.dot_general(hidden, down_local, (((0,), (0,)), ((), ())), preferred_element_type=F32)
    summed = lax.psum_scatter(mixed, "ra", scatter_dimension=0, tiled=True)
    stream = 0.1 * inputs + summed * down_scale
    second = lax.psum(jnp.sum(stream * stream, axis=1), "cb")
    rscale_second = lax.rsqrt(second / features + EPS)[:, None]
    return (stream * rscale_second * gain_second).astype(BF16)


def solution(mesh):
    placed = (
        P("ra", "cb"),
        P("cb"),
        P("ra", "cb"),
        P("ra"),
        P("ra", "cb"),
        P("ra"),
        P("ra", "cb"),
        P("cb"),
        P("cb"),
    )
    planes = mesh.shape["ra"] // 4
    paired = mesh.shape["cb"] == 2 and planes >= 2 and planes & (planes - 1) == 0
    body = functools.partial(fused, planes) if paired else plain
    return jax.shard_map(
        body, mesh=mesh, in_specs=placed, out_specs=P("ra", "cb"), check_vma=False
    )
```

```python
import functools

import jax
import jax.numpy as jnp
from jax import lax
from jax.experimental import pallas as pl
from jax.experimental.pallas import tpu as pltpu
from jax.sharding import PartitionSpec as P

EPS = 1e-06
MESH = pl.DeviceIdType.MESH
F32 = jnp.float32
BF16 = jnp.bfloat16


def flip(index, mask):
    bit = 1
    while bit <= mask:
        if mask & bit:
            index = index + (1 - 2 * ((index // bit) % 2)) * bit
        bit *= 2
    return index


def kernel(
    planes,
    features,
    x_ref,
    gain_ref,
    gate_hbm,
    gate_scale_ref,
    up_hbm,
    up_scale_ref,
    down_hbm,
    down_scale_ref,
    gain2_ref,
    out_ref,
    wide,
    gate_w,
    up_w,
    down_w,
    xg,
    scaled,
    hidden,
    part,
    ex_send,
    ex_recv,
    sq_send,
    sq_recv,
    keep_a,
    keep_b,
    send_a,
    send_b,
    recv_a,
    recv_b,
    send2_a,
    send2_b,
    recv2_a,
    recv2_b,
    own_sum,
    z_send,
    z_recv,
    last_send,
    last_recv,
    w_sem,
    ssem,
    rsem,
):
    ra = lax.axis_index("ra")
    cb = lax.axis_index("cb")
    rows, width = x_ref.shape
    half = width // 2
    x_peer = (flip(ra, 1), cb)
    y_peer = (flip(ra, 2), cb)
    z_peers = [None] + [(flip(ra, 4 * k), cb) for k in range(1, planes)]
    core_peer = (ra, flip(cb, 1))
    first, second = pl.ds(0, half), pl.ds(half, half)

    loads = []
    for i, src in enumerate((gate_hbm, up_hbm, down_hbm)):
        load = pltpu.make_async_copy(src, wide.at[i], w_sem.at[i])
        load.start()
        loads.append(load)

    barrier = pltpu.get_barrier_semaphore()
    peers = [x_peer, y_peer, core_peer] + z_peers[1:]
    for peer in peers:
        pl.semaphore_signal(barrier, inc=1, device_id=peer, device_id_type=MESH)
    pl.semaphore_wait(barrier, len(peers))

    copies = {}

    def send(name, k, src, dst, peer):
        slot = len(copies)
        copy = pltpu.make_async_remote_copy(
            src_ref=src,
            dst_ref=dst,
            send_sem=ssem.at[slot],
            recv_sem=rsem.at[slot],
            device_id=peer,
            device_id_type=MESH,
        )
        copy.start()
        copies[name, k] = copy

    def arrived(name, k):
        copies[name, k].wait_recv()

    halves = (first, second)

    def spread(k):
        for i in (1, 0):
            if k:
                arrived(("z", i), k)
            for name, slot, peer in (("gx", 1, x_peer), ("gy", 2, y_peer)):
                h = i if k or name == "gx" else 1 - i
                src = (xg.at[k, 0] if k else x_ref).at[:, halves[h]]
                send((name, h), k, src, xg.at[k, slot, :, halves[h]], peer)

    def forward(k):
        arrived(("gx", 1), k)
        send("fy", k, xg.at[k, 1, :, second], xg.at[k, 3, :, second], y_peer)
        arrived(("gy", 0), k)
        send("fx", k, xg.at[k, 2, :, first], xg.at[k, 3, :, first], x_peer)

    nt = (((1,), (1,)), ((), ()))

    def gate_up(k):
        arrived(("gx", 0), k)
        arrived(("gy", 1), k)
        arrived("fx", k)
        arrived("fy", k)

        def prepare(s, carry):
            block = xg[k, s].astype(F32)
            squares = jnp.sum(block * block, axis=1, keepdims=True)
            sq_send[k, s] = jnp.broadcast_to(squares, (rows, 128))
            scaled[s] = (block * gain_ref[...]).astype(BF16)
            return carry

        lax.fori_loop(0, 4, prepare, 0)
        send("sq", k, sq_send.at[k], sq_recv.at[k], core_peer)
        tokens = scaled[...].reshape(4 * rows, width)
        for i, w in enumerate((gate_w, up_w)):
            product = lax.dot_general(tokens, w[...], nt, preferred_element_type=F32)
            part[k, i] = product
            ex_send[k, i] = product.astype(BF16)
            send(("ex", i), k, ex_send.at[k, i], ex_recv.at[k, i], core_peer)

    def down(k):
        arrived("sq", k)
        arrived(("ex", 0), k)
        arrived(("ex", 1), k)

        for s in range(4):
            here = slice(s * rows, (s + 1) * rows)
            squares = (sq_send[k, s] + sq_recv[k, s])[:, :1]
            rscale = lax.rsqrt(squares / features + EPS)
            gate = (part[k, 0, here] + ex_recv[k, 0, here].astype(F32)) * rscale * gate_scale_ref[...][None, :]
            up = (part[k, 1, here] + ex_recv[k, 1, here].astype(F32)) * rscale * up_scale_ref[...][None, :]
            hidden[here] = (gate / (1.0 + jnp.exp(-gate)) * up).astype(BF16)
        units = hidden[...]
        prod = jnp.dot(units, down_w[:, :half], preferred_element_type=F32)
        for dy in range(2):
            low = 2 * dy * rows
            keep_a[k, dy] = prod[low : low + rows]
            send_a[k, dy] = prod[low + rows : low + 2 * rows].astype(BF16)
        prod = jnp.dot(units, down_w[:, half:], preferred_element_type=F32)
        for dx in range(2):
            low = dx * rows
            keep_b[k, dx] = prod[low : low + rows]
            low += 2 * rows
            send_b[k, dx] = prod[low : low + rows].astype(BF16)

    def issue(k):
        send("a1", k, send_a.at[k], recv_a.at[k], x_peer)
        send("b1", k, send_b.at[k], recv_b.at[k], y_peer)

    def reduce_one(k):
        arrived("a1", k)
        send2_a[k] = (keep_a[k, 1] + recv_a[k, 1].astype(F32)).astype(BF16)
        send("a2", k, send2_a.at[k], recv2_a.at[k], y_peer)
        arrived("b1", k)
        send2_b[k] = (keep_b[k, 1] + recv_b[k, 1].astype(F32)).astype(BF16)
        send("b2", k, send2_b.at[k], recv2_b.at[k], x_peer)

    def reduce_two(k):
        arrived("a2", k)
        sum_a = keep_a[k, 0] + recv_a[k, 0].astype(F32) + recv2_a[k].astype(F32)
        arrived("b2", k)
        sum_b = keep_b[k, 0] + recv_b[k, 0].astype(F32) + recv2_b[k].astype(F32)
        if k == 0:
            own_sum[:, :half] = sum_a
            own_sum[:, half:] = sum_b
        else:
            z_send[k, :, :half] = sum_a.astype(BF16)
            z_send[k, :, half:] = sum_b.astype(BF16)
            send("zs", k, z_send.at[k], z_recv.at[k], z_peers[k])

    def narrow(i, target):
        loads[i].wait()
        step = 64

        def body(j, carry):
            here = pl.ds(pl.multiple_of(j * step, step), step)
            target[here] = wide[i, here].astype(BF16)
            return carry

        lax.fori_loop(0, target.shape[0] // step, body, 0)

    spread(0)
    for k in range(1, planes):
        for i in (1, 0):
            part_of = pl.ds(i * half, half)
            send(("z", i), k, x_ref.at[:, part_of], xg.at[k, 0, :, part_of], z_peers[k])
    xg[0, 0] = x_ref[...]
    forward(0)
    spread(1)
    narrow(0, gate_w)
    narrow(1, up_w)
    gate_up(0)
    forward(1)
    for k in range(1, planes):
        if k + 1 < planes:
            spread(k + 1)
        if k == 1:
            narrow(2, down_w)
        if k > 2:
            down(k - 1)
            issue(k - 1)
        elif k == 2:
            down(1)
            issue(1)
        gate_up(k)
        if k + 1 < planes:
            forward(k + 1)
    late = list(range(1, planes)) + [0]
    down(0)
    if planes > 2:
        reduce_one(1)
    down(planes - 1)
    issue(planes - 1)
    issue(0)
    if planes == 2:
        reduce_one(1)
    for at in range(1, planes):
        reduce_one(late[at])
        reduce_two(late[at - 1])
    reduce_two(0)

    total = own_sum[...]
    for k in range(1, planes):
        arrived("zs", k)
        total = total + z_recv[k].astype(F32)
    stream = 0.1 * x_ref[...].astype(F32) + total * down_scale_ref[...]
    own_sum[...] = stream
    last_send[...] = jnp.broadcast_to(
        jnp.sum(stream * stream, axis=1, keepdims=True), last_send.shape
    )
    send("last", 0, last_send, last_recv, core_peer)
    arrived("last", 0)
    both = (last_send[...] + last_recv[...])[:, :1]
    rscale = lax.rsqrt(both / features + EPS)
    out_ref[...] = (own_sum[...] * rscale * gain2_ref[...]).astype(BF16)
    for copy in copies.values():
        copy.wait_send()


def fused(
    planes,
    activations,
    gain_first,
    gate_weight,
    gate_scale,
    up_weight,
    up_scale,
    down_weight,
    down_scale,
    gain_second,
):
    rows, width = activations.shape
    units = gate_weight.shape[0]
    half = width // 2
    group = 4 * rows
    n_copies = 20 * planes
    vmem = pl.BlockSpec(memory_space=pltpu.VMEM)
    hbm = pl.BlockSpec(memory_space=pl.ANY)
    scratch = [
        pltpu.VMEM((3, units, width), F32),
        pltpu.VMEM((units, width), BF16),
        pltpu.VMEM((units, width), BF16),
        pltpu.VMEM((units, width), BF16),
        pltpu.VMEM((planes, 4, rows, width), BF16),
        pltpu.VMEM((4, rows, width), BF16),
        pltpu.VMEM((group, units), BF16),
        pltpu.VMEM((planes, 2, group, units), F32),
        pltpu.VMEM((planes, 2, group, units), BF16),
        pltpu.VMEM((planes, 2, group, units), BF16),
        pltpu.VMEM((planes, 4, rows, 128), F32),
        pltpu.VMEM((planes, 4, rows, 128), F32),
        pltpu.VMEM((planes, 2, rows, half), F32),
        pltpu.VMEM((planes, 2, rows, half), F32),
        pltpu.VMEM((planes, 2, rows, half), BF16),
        pltpu.VMEM((planes, 2, rows, half), BF16),
        pltpu.VMEM((planes, 2, rows, half), BF16),
        pltpu.VMEM((planes, 2, rows, half), BF16),
        pltpu.VMEM((planes, rows, half), BF16),
        pltpu.VMEM((planes, rows, half), BF16),
        pltpu.VMEM((planes, rows, half), BF16),
        pltpu.VMEM((planes, rows, half), BF16),
        pltpu.VMEM((rows, width), F32),
        pltpu.VMEM((planes, rows, width), BF16),
        pltpu.VMEM((planes, rows, width), BF16),
        pltpu.VMEM((rows, 128), F32),
        pltpu.VMEM((rows, 128), F32),
        pltpu.SemaphoreType.DMA((3,)),
        pltpu.SemaphoreType.DMA((n_copies,)),
        pltpu.SemaphoreType.DMA((n_copies,)),
    ]
    return pl.pallas_call(
        functools.partial(kernel, planes, width * 2),
        out_shape=jax.ShapeDtypeStruct((rows, width), BF16),
        in_specs=[vmem, vmem, hbm, vmem, hbm, vmem, hbm, vmem, vmem],
        out_specs=vmem,
        scratch_shapes=scratch,
        compiler_params=pltpu.CompilerParams(
            collective_id=0, has_side_effects=True, vmem_limit_bytes=60 * 1024 * 1024
        ),
    )(
        activations,
        gain_first[None, :],
        gate_weight,
        gate_scale,
        up_weight,
        up_scale,
        down_weight,
        down_scale[None, :],
        gain_second[None, :],
    )


def plain(
    activations,
    gain_first,
    gate_weight,
    gate_scale,
    up_weight,
    up_scale,
    down_weight,
    down_scale,
    gain_second,
):
    inputs = activations.astype(F32)
    features = activations.shape[1] * lax.axis_size("cb")
    gate_local = gate_weight.astype(BF16)
    up_local = up_weight.astype(BF16)
    down_local = down_weight.astype(BF16)
    gathered = lax.all_gather(activations, "ra", axis=0, tiled=True)
    wide_rows = gathered.astype(F32)
    row_squares = jnp.sum(wide_rows * wide_rows, axis=1)
    scaled = (wide_rows * gain_first).astype(BF16)
    contract = (((1,), (1,)), ((), ()))
    squares = lax.psum(row_squares, "cb")
    gate_part = lax.dot_general(gate_local, scaled, contract, preferred_element_type=F32)
    up_part = lax.dot_general(up_local, scaled, contract, preferred_element_type=F32)
    gate_sum, up_sum = lax.psum((gate_part, up_part), "cb")
    rscale_first = lax.rsqrt(squares / features + EPS)[None, :]
    gate_full = gate_sum * rscale_first * gate_scale[:, None]
    up_full = up_sum * rscale_first * up_scale[:, None]
    hidden = (jax.nn.silu(gate_full) * up_full).astype(BF16)
    mixed = lax.dot_general(hidden, down_local, (((0,), (0,)), ((), ())), preferred_element_type=F32)
    summed = lax.psum_scatter(mixed, "ra", scatter_dimension=0, tiled=True)
    stream = 0.1 * inputs + summed * down_scale
    second = lax.psum(jnp.sum(stream * stream, axis=1), "cb")
    rscale_second = lax.rsqrt(second / features + EPS)[:, None]
    return (stream * rscale_second * gain_second).astype(BF16)


def solution(mesh):
    placed = (
        P("ra", "cb"),
        P("cb"),
        P("ra", "cb"),
        P("ra"),
        P("ra", "cb"),
        P("ra"),
        P("ra", "cb"),
        P("cb"),
        P("cb"),
    )
    planes = mesh.shape["ra"] // 4
    paired = mesh.shape["cb"] == 2 and planes >= 2 and planes & (planes - 1) == 0
    body = functools.partial(fused, planes) if paired else plain
    return jax.shard_map(
        body, mesh=mesh, in_specs=placed, out_specs=P("ra", "cb"), check_vma=False
    )
```
